32 devices in a mesh: fs: 4 (over z), rep: 4 (over y, x), tp: 2 (over core).
Axes of the slice: x: 2, y: 2, z: 4, core: 2. Of those that a mesh axis runs over, the one named last changes fastest.
Arguments:
- tokens_in: bfloat16 [8192, 2048], P(('fs', 'rep')), may hold values from -6 to 6
- query_two: bfloat16 [8192, 512], P(('fs', 'rep'), 'tp'), may hold values from -49 to 49
- key_two: bfloat16 [8192, 512], P(('fs', 'rep'), 'tp'), may hold values from -9 to 9
- values: bfloat16 [8192, 1024], P(('fs', 'rep'), 'tp'), may hold values from -6 to 6
- out_grad: bfloat16 [8192, 1024], P(('fs', 'rep'), 'tp'), may hold values from -6 to 6
- second_scale: float32 [8], P('tp'), may hold values from 0.3 to 0.8
- factor: bfloat16 [2048, 256], P('fs'), may hold values from -0.125 to 0.125
- weight: float32 [2048, 512], P('fs', 'tp'), may hold values from -0.6 to 0.6
- first_moment: float32 [256, 512], P('fs', 'tp'), may hold values from -135.7645 to 135.7645
- second_moment: float32 [256, 512], P('fs', 'tp'), may hold values from 5 to 8192
Outputs:
- new_weight: float32 [2048, 512], P('fs', 'tp')
- weight_copy: bfloat16 [2048, 512], P(None, 'tp')
- update_step: float32 [2048, 512], P('fs', 'tp')
- new_first: float32 [256, 512], P('fs', 'tp')
- new_second: float32 [256, 512], P('fs', 'tp')
The draws below stay inside these ranges and needn't reach their ends.
All inputs are finite; a program needn't handle non-finite values.
Results may differ from the reference program's by a relative error of at most 0.006.
Values may be sent and summed in bfloat16 or wider, within the bound.
A program may use at most 64 MiB of HBM per device.

```python
import jax
import jax.numpy as jnp
from jax import lax

D = 2048
HEADS_W = 8
VD = 128
RANK = 256
TOK_DEV = 512
KW = 512
TOKENS = 8192


def drawn_pair(key):
    base = jax.random.fold_in(key, 11)
    key_query, key_keys = jax.random.split(base, 2)
    queries = jnp.clip(1.4 * jax.random.normal(key_query, (TOKENS, KW), jnp.float32), -8.4, 8.4)
    keys_all = jnp.clip(1.4 * jax.random.normal(key_keys, (TOKENS, KW), jnp.float32), -8.4, 8.4)
    return (queries, keys_all)


def draw_query_two(key, part):
    return drawn_pair(key)[0].astype(jnp.bfloat16)


def draw_key_two(key, part):
    return drawn_pair(key)[1].astype(jnp.bfloat16)


def draw_first_moment(key, part):
    base = jax.random.fold_in(key, 23)
    moment_scale = 0.25 * TOKENS ** 0.5
    raw_values = jnp.clip(jax.random.normal(base, (RANK, KW), jnp.float32), -6.0, 6.0)
    return moment_scale * raw_values


def draw_second_moment(key, part):
    base = jax.random.fold_in(key, 37)
    rank_index = jnp.arange(RANK, dtype=jnp.float32)[:, None]
    falling = 100.0 ** (-rank_index / max(RANK - 1, 1))
    jitter = jnp.exp(jax.random.uniform(base, (RANK, KW), jnp.float32, -0.693, 0.693))
    return 0.25 * TOKENS * falling * jitter


def with_spikes(values, rng, source, target, shards_of, factor):
    owner, partner = [(jnp.arange(values.shape[dim]) // (values.shape[dim] // shards_of)).reshape([-1 if axis == dim else 1 for axis in range(values.ndim)]) for dim in (source, target)]
    chosen = jax.random.permutation(rng, shards_of)[partner]
    strong = (owner == chosen) | (owner == (partner + shards_of // 2) % shards_of)
    return jnp.where(strong, factor * values, values)


def block_levels(own_key, dims, cuts, least, top_value):
    gain, own = 1.0, jax.random.fold_in(own_key, 6)
    for dim, shards_of in cuts:
        draws = jnp.exp(jax.random.uniform(jax.random.fold_in(own, dim), (shards_of,), jnp.float32, least / len(cuts), top_value / len(cuts)))
        gain = gain * jnp.repeat(draws, dims[dim] // shards_of).reshape([-1 if axis == dim else 1 for axis in range(len(dims))])
    return gain


def noise(key, extent, width, most, cuts=(), kind=jnp.bfloat16):
    array = jax.random.normal(key, extent, jnp.float32) * width
    if len(cuts) > 0:
        array = block_levels(key, extent, cuts, -0.22, 0.18) * array
    return jnp.clip(array, min=-most, max=most).astype(kind)


def heavy_noise(own_key, shape, spread, most, cuts, heavy, held_as=jnp.bfloat16):
    values = spread * jax.random.normal(own_key, shape, jnp.float32)
    if cuts:
        values = values * block_levels(own_key, shape, cuts, -0.22, 0.18)
    return jnp.clip(with_spikes(values, jax.random.fold_in(own_key, 3), *heavy), -most, most).astype(held_as)


def setup_inputs(seed: int = 0) -> dict:
    keys = jax.random.split(jax.random.key(seed), 11)
    return {
        "tokens_in": heavy_noise(keys[0], (TOKENS, D), 1.0, 6.0, ((0, 16),), (0, 1, 16, 2.0)),
        "query_two": draw_query_two(jax.random.fold_in(keys[10], 71), 0),
        "key_two": draw_key_two(jax.random.fold_in(keys[10], 71), 0),
        "values": noise(keys[3], (TOKENS, HEADS_W * VD), 1.0, 6.0, ((0, 16), (1, 2))),
        "out_grad": noise(keys[4], (TOKENS, HEADS_W * VD), 1.0, 6.0, ((0, 16), (1, 2))),
        "second_scale": jnp.clip(0.3 + 0.5 * jax.random.uniform(keys[5], (HEADS_W,), jnp.float32) ** block_levels(keys[5], (HEADS_W,), ((0, 2),), -0.2, 0.2), 0.3, 0.8),
        "factor": noise(keys[6], (D, RANK), D ** -0.5, 0.125, ((0, 4),)),
        "weight": noise(keys[7], (D, KW), 0.1, 0.6, ((0, 4), (1, 2)), jnp.float32),
        "first_moment": draw_first_moment(jax.random.fold_in(keys[10], 71), 0),
        "second_moment": draw_second_moment(jax.random.fold_in(keys[10], 71), 0),
    }


def key_gradient(query_rows, key_rows, value_rows, grad_rows, second_scale):
    length = query_rows.shape[0]
    head_count = second_scale.shape[0]
    queries = query_rows.astype(jnp.float32).reshape(length, head_count, -1)
    keys_all = key_rows.astype(jnp.float32).reshape(length, head_count, -1)
    value_heads = value_rows.astype(jnp.float32).reshape(length, head_count, -1)
    grad_heads = grad_rows.astype(jnp.float32).reshape(length, head_count, -1)
    inv_root = queries.shape[2] ** (-0.5)
    scores = jnp.einsum('qhd,khd->hqk', queries, keys_all) * inv_root
    positions = jnp.arange(length, dtype=jnp.int32)
    causal = positions[:, None] >= positions[None, :]
    scores = jnp.where(causal[None], scores, -1e+30)
    row_peak = lax.optimization_barrier(jnp.max(scores, axis=-1, keepdims=True))
    exps = jnp.exp(scores - row_peak)
    weights_map = exps / lax.optimization_barrier(jnp.sum(exps, axis=-1, keepdims=True))
    attn_grad = jnp.einsum('qhe,khe->hqk', grad_heads, value_heads)
    row_inner = lax.optimization_barrier(jnp.sum(weights_map * attn_grad, axis=-1, keepdims=True))
    score_grad = ((-second_scale)[:, None, None] * weights_map * (attn_grad - row_inner)).astype(jnp.bfloat16)
    score_grad = lax.optimization_barrier(score_grad)
    key_grad = jnp.einsum('hqk,qhd->khd', score_grad.astype(jnp.float32), queries) * inv_root
    return key_grad.reshape(length, -1).astype(jnp.bfloat16)

def reference(tokens_in, query_two, key_two, values, out_grad, second_scale, factor, weight, first_moment, second_moment):
    sequences = TOKENS // TOK_DEV

    def accumulate(running, pieces):
        token_rows, query_rows, key_rows, value_rows, grad_rows = pieces
        key_grad = key_gradient(query_rows, key_rows, value_rows, grad_rows, second_scale)
        return (running + jnp.dot(token_rows.T, key_grad, preferred_element_type=jnp.float32), None)
    pieces = (tokens_in.reshape(sequences, TOK_DEV, D), query_two.reshape(sequences, TOK_DEV, KW), key_two.reshape(sequences, TOK_DEV, KW), values.reshape(sequences, TOK_DEV, HEADS_W * VD), out_grad.reshape(sequences, TOK_DEV, HEADS_W * VD))
    gradient, unused_out = lax.scan(accumulate, jnp.zeros((D, KW), jnp.float32), pieces)
    projected = jnp.dot(factor.astype(jnp.float32).T, gradient, precision=lax.Precision.HIGHEST)
    new_first = 0.9 * first_moment + 0.1 * projected
    new_second = 0.95 * second_moment + 0.05 * projected * projected
    direction = (new_first / (jnp.sqrt(new_second) + 1e-08)).astype(jnp.bfloat16)
    squares = jnp.sum(jnp.square(lax.optimization_barrier(direction).astype(jnp.float32)))
    update_step = jnp.dot(factor, direction, preferred_element_type=jnp.float32) * lax.rsqrt(squares / (RANK * KW) + 1e-06)
    new_weight = weight - 0.1 * update_step
    return (new_weight, new_weight.astype(jnp.bfloat16), update_step, new_first, new_second)
```

```python
import functools

import jax
import jax.numpy as jnp
from jax import lax
from jax.experimental import pallas as pl
from jax.experimental.pallas import tpu as pltpu
from jax.sharding import PartitionSpec as P

MESH = pl.DeviceIdType.MESH
LANES = 128
NT = (((1,), (1,)), ((), ()))
TN = (((0,), (0,)), ((), ()))


def attention_pair(pair, q_v, k_v, v_v, g_v, scale_ref, acc, kgb, head_width):
    length = q_v.shape[0]
    per = LANES // head_width
    block = min(LANES, length)
    cols = slice(pair * LANES, (pair + 1) * LANES)
    value_width = v_v.shape[1] // (q_v.shape[1] // head_width)
    lane = lax.broadcasted_iota(jnp.int32, (length, LANES), 1)
    tri = lax.broadcasted_iota(jnp.int32, (block, block), 0) <= lax.broadcasted_iota(
        jnp.int32, (block, block), 1
    )
    for inner_head in range(per):
        head = pair * per + inner_head
        in_head = (lane >= inner_head * head_width) & (lane < (inner_head + 1) * head_width)
        queries = jnp.where(in_head, q_v[:, cols].astype(jnp.float32) * head_width ** (-0.5), 0.0)
        queries = queries.astype(jnp.bfloat16)
        vcols = slice(head * value_width, (head + 1) * value_width)
        scale = scale_ref[head]
        for at in reversed(range(length // block)):
            keys_to = (at + 1) * block
            rows = slice(at * block, keys_to)
            qb = queries[rows]
            s = lax.dot_general(k_v[:keys_to, cols], qb, NT, preferred_element_type=jnp.float32)
            last = jnp.where(tri, s[at * block :], -1e30)
            s = last if at == 0 else jnp.concatenate([s[: at * block], last], axis=0)
            e = jnp.exp(s - jnp.max(s, axis=0, keepdims=True))
            inv = 1.0 / jnp.sum(e, axis=0, keepdims=True)
            a = lax.dot_general(
                v_v[:keys_to, vcols], g_v[rows, vcols], NT, preferred_element_type=jnp.float32
            )
            row_inner = jnp.sum(e * a, axis=0, keepdims=True) * inv
            sg = (e * (a - row_inner) * (-scale * inv)).astype(jnp.bfloat16)
            add = jnp.dot(sg, qb, preferred_element_type=jnp.float32)
            if inner_head == 0 and at == length // block - 1:
                acc[...] = add
            else:
                acc[:keys_to] += add
    kgb[:, cols] = acc[...].astype(jnp.bfloat16)


def main_kernel(
    fs, rep, tp, head_width,
    scale_ref, tok_h, q_h, k_h, v_h, g_h, factor_h, weight_h, first_h, second_h,
    fac, wbf, dirs, proj, sq_out,
    tok, q_v, k_v, v_v, g_v, wq, wsend, fm, sm, acc, kgb, red, psend, precv, sq_own, sq_in,
    ld, fac_s, fac_r, par_s, par_r, w_s, w_r, wf_s, wf_r, pc_s, pc_r, dr_s, dr_r, pj_s, pj_r, sq_s, sq_r,
):
    n = fs * rep
    z, r, c = lax.axis_index("fs"), lax.axis_index("rep"), lax.axis_index("tp")
    me = z * rep + r
    other = lax.rem(c + 1, tp)
    partner = {"fs": z, "rep": r, "tp": other}
    half = fac.shape[2] // tp
    my_cols = pl.ds(pl.multiple_of(c * half, half), half)
    his_cols = pl.ds(pl.multiple_of(other * half, half), half)

    def remote(src, dst, send, recv, device):
        return pltpu.make_async_remote_copy(
            src_ref=src, dst_ref=dst, send_sem=send, recv_sem=recv, device_id=device, device_id_type=MESH
        )

    def fs_dev(i):
        return {"fs": i, "rep": r, "tp": c}

    def rep_dev(i):
        return {"fs": z, "rep": i, "tp": c}

    def any_dev(i):
        return {"fs": i // rep, "rep": lax.rem(i, rep), "tp": c}

    def each(count, body):
        def step(d, carry):
            body(d)
            return carry

        lax.fori_loop(1, count, step, 0)

    barrier = pltpu.get_barrier_semaphore()
    pl.semaphore_signal(barrier, inc=1, device_id=partner, device_id_type=MESH)

    def greet(d):
        pl.semaphore_signal(barrier, inc=1, device_id=any_dev(lax.rem(me + d, n)), device_id_type=MESH)

    each(n, greet)

    loads = [
        pltpu.make_async_copy(src, dst, ld.at[i])
        for i, (src, dst) in enumerate(
            [
                (factor_h, fac.at[z]), (weight_h.at[r], wq), (q_h, q_v), (k_h, k_v), (v_h, v_v), (g_h, g_v),
                (tok_h, tok), (first_h.at[r], fm), (second_h.at[r], sm),
            ]
        )
    ]
    for load in loads:
        load.start()
    loads[1].wait()
    wsend[...] = wq[...].astype(jnp.bfloat16)
    loads[0].wait()
    pl.semaphore_wait(barrier, n)

    def fac_copy(slot, sem, to):
        part = fac.at[slot, :, my_cols]
        return remote(part, part, fac_s.at[sem], fac_r.at[slot], fs_dev(to))

    def send_fac(d):
        fac_copy(z, d, lax.rem(z + d, fs)).start()

    each(fs, send_fac)

    def w_copy(slot, sem, to):
        return remote(wsend, wbf.at[slot, r], w_s.at[sem], w_r.at[slot], fs_dev(to))

    def send_w(d):
        w_copy(z, d, lax.rem(z + d, fs)).start()

    each(fs, send_w)

    for i in range(2, 6):
        loads[i].wait()
    for pair in range(q_v.shape[1] // LANES):
        attention_pair(pair, q_v, k_v, v_v, g_v, scale_ref, acc, kgb, head_width)
    for i in range(6, 9):
        loads[i].wait()

    by_shard = fac.shape[1] % LANES == 0

    def tokens_of(j):
        return tok[:, pl.ds(pl.multiple_of(j * fac.shape[1], LANES), fac.shape[1])]

    if by_shard:
        red[...] = jnp.dot(tokens_of(z), fac[z], preferred_element_type=jnp.float32)

    def par_copy(slot, cols):
        part = fac.at[slot, :, cols]
        return remote(part, part, par_s.at[slot], par_r.at[slot], partner)

    def forward_fac(d):
        src = lax.rem(z + d, fs)
        fac_copy(src, d, src).wait_recv()
        par_copy(src, my_cols).start()

    each(fs, forward_fac)

    def use_fac(d):
        src = lax.rem(z + d, fs)
        par_copy(src, his_cols).wait_recv()
        if by_shard:
            red[...] += jnp.dot(tokens_of(src), fac[src], preferred_element_type=jnp.float32)

    each(fs, use_fac)
    if not by_shard:
        whole = jnp.concatenate([fac[j] for j in range(fs)], axis=0)
        red[...] = jnp.dot(tok[...], whole, preferred_element_type=jnp.float32)

    partial = lax.dot_general(
        red[...].astype(jnp.bfloat16), kgb[...], TN, preferred_element_type=jnp.float32
    )
    piece = psend.shape[1]
    for i in range(n):
        psend[i] = partial[i * piece : (i + 1) * piece].astype(jnp.bfloat16)

    def pc_copy(part, slot, sem, to):
        return remote(psend.at[part], precv.at[slot], pc_s.at[sem], pc_r.at[slot], any_dev(to))

    def send_piece(d):
        to = lax.rem(me + d, n)
        pc_copy(to, me, d, to).start()

    each(n, send_piece)

    def wf_copy(slot, lane, sem, to):
        part = wbf.at[slot, lane]
        return remote(part, part, wf_s.at[slot, sem], wf_r.at[slot, lane], rep_dev(to))

    def relay_w(d):
        src = lax.rem(z + d, fs)
        w_copy(src, d, src).wait_recv()
        each(rep, lambda k: wf_copy(src, r, k, lax.rem(r + k, rep)).start())

    each(fs, relay_w)

    def wait_piece(d):
        src = lax.rem(me + d, n)
        pc_copy(src, src, d, src).wait_recv()

    each(n, wait_piece)
    precv[me] = psend[me]
    total = jnp.sum(precv[...].astype(jnp.float32), axis=0)
    first = 0.9 * fm[...] + 0.1 * total
    second = 0.95 * sm[...] + 0.05 * total * total
    dirs[me] = (first / (jnp.sqrt(second) + 1e-08)).astype(jnp.bfloat16)
    proj[r] = total

    def dr_copy(slot, sem, to):
        part = dirs.at[slot]
        return remote(part, part, dr_s.at[sem], dr_r.at[slot], any_dev(to))

    def pj_copy(slot, sem, to):
        part = proj.at[slot]
        return remote(part, part, pj_s.at[sem], pj_r.at[slot], rep_dev(to))

    each(n, lambda d: dr_copy(me, d, lax.rem(me + d, n)).start())
    each(rep, lambda d: pj_copy(r, d, lax.rem(r + d, rep)).start())

    def wait_dir(d):
        src = lax.rem(me + d, n)
        dr_copy(src, d, src).wait_recv()

    each(n, wait_dir)
    wide = dirs[...].astype(jnp.float32)
    sq_own[...] = jnp.full(sq_own.shape, jnp.sum(wide * wide), jnp.float32)
    sq_copy = remote(sq_own, sq_in, sq_s, sq_r, partner)
    sq_copy.start()

    def wait_proj(d):
        src = lax.rem(r + d, rep)
        pj_copy(src, d, src).wait_recv()

    each(rep, wait_proj)

    def wait_relay(d):
        src = lax.rem(z + d, fs)

        def inner(k):
            lane = lax.rem(r + k, rep)
            wf_copy(src, lane, k, lane).wait_recv()

        each(rep, inner)

    each(fs, wait_relay)

    def wait_sends_fs(d):
        src = lax.rem(z + d, fs)
        fac_copy(z, d, src).wait_send()
        w_copy(z, d, src).wait_send()
        par_copy(src, my_cols).wait_send()
        each(rep, lambda k: wf_copy(src, r, k, lax.rem(r + k, rep)).wait_send())

    each(fs, wait_sends_fs)

    def wait_sends_all(d):
        to = lax.rem(me + d, n)
        pc_copy(to, me, d, to).wait_send()
        dr_copy(me, d, to).wait_send()

    each(n, wait_sends_all)
    each(rep, lambda d: pj_copy(r, d, lax.rem(r + d, rep)).wait_send())
    sq_copy.wait()
    sq_out[...] = sq_own[...] + sq_in[...]


def end_kernel(
    fs, entries,
    sq, factor, direction, fac, wbf, weight, proj, fm, sm,
    new_weight, copies, update, new_first, new_second,
):
    z = lax.axis_index("fs")
    rows = factor.shape[0]
    ratio = lax.rsqrt(sq[0:1, 0:1] / entries + 1e-06)
    own = jnp.dot(factor[...], direction[...], preferred_element_type=jnp.float32) * ratio
    update[...] = own
    changed = weight[...] - 0.1 * own
    new_weight[...] = changed
    copies[pl.ds(pl.multiple_of(z * rows, rows), rows), :] = changed.astype(jnp.bfloat16)
    for d in range(1, fs):
        at = pl.ds(pl.multiple_of(lax.rem(z + d, fs) * rows, rows), rows)
        step = jnp.dot(fac[at, :], direction[...], preferred_element_type=jnp.float32) * ratio
        copies[at, :] = (wbf[at, :].astype(jnp.float32) - 0.1 * step).astype(jnp.bfloat16)
    total = proj[...]
    new_first[...] = 0.9 * fm[...] + 0.1 * total
    new_second[...] = 0.95 * sm[...] + 0.05 * total * total


def on_device(
    fs, rep, tp,
    tokens_in, query_two, key_two, values, out_grad, second_scale, factor, weight, first_moment, second_moment,
):
    n = fs * rep
    length, width = query_two.shape
    head_width = width // second_scale.shape[0]
    rows, rank = factor.shape
    own_rows = first_moment.shape[0]
    piece = own_rows // rep
    w_rows = rows // rep
    f32, bf16 = jnp.float32, jnp.bfloat16
    any_spec = pl.BlockSpec(memory_space=pl.ANY)
    vmem = pl.BlockSpec(memory_space=pltpu.VMEM)
    dma = pltpu.SemaphoreType.DMA
    fac, wbf, dirs, proj, sq = pl.pallas_call(
        functools.partial(main_kernel, fs, rep, tp, head_width),
        out_shape=(
            jax.ShapeDtypeStruct((fs, rows, rank), bf16),
            jax.ShapeDtypeStruct((fs, rep, w_rows, width), bf16),
            jax.ShapeDtypeStruct((n, piece, width), bf16),
            jax.ShapeDtypeStruct((rep, piece, width), f32),
            jax.ShapeDtypeStruct((8, LANES), f32),
        ),
        in_specs=[pl.BlockSpec(memory_space=pltpu.SMEM)] + [any_spec] * 9,
        out_specs=(vmem,) * 5,
        scratch_shapes=[
            pltpu.VMEM(tokens_in.shape, bf16),
            pltpu.VMEM(query_two.shape, bf16),
            pltpu.VMEM(key_two.shape, bf16),
            pltpu.VMEM(values.shape, bf16),
            pltpu.VMEM(out_grad.shape, bf16),
            pltpu.VMEM((w_rows, width), f32),
            pltpu.VMEM((w_rows, width), bf16),
            pltpu.VMEM((piece, width), f32),
            pltpu.VMEM((piece, width), f32),
            pltpu.VMEM((length, LANES), f32),
            pltpu.VMEM((length, width), bf16),
            pltpu.VMEM((length, rank), f32),
            pltpu.VMEM((n, piece, width), bf16),
            pltpu.VMEM((n, piece, width), bf16),
            pltpu.VMEM((8, LANES), f32),
            pltpu.VMEM((8, LANES), f32),
            dma((9,)),
            dma((fs,)), dma((fs,)),
            dma((fs,)), dma((fs,)),
            dma((fs,)), dma((fs,)),
            dma((fs, rep)), dma((fs, rep)),
            dma((n,)), dma((n,)),
            dma((n,)), dma((n,)),
            dma((rep,)), dma((rep,)),
            dma, dma,
        ],
        compiler_params=pltpu.CompilerParams(
            collective_id=0, has_side_effects=True, vmem_limit_bytes=48 * 1024 * 1024
        ),
        name="main_kernel",
    )(
        second_scale, tokens_in, query_two, key_two, values, out_grad, factor,
        weight.reshape(rep, w_rows, width),
        first_moment.reshape(rep, piece, width),
        second_moment.reshape(rep, piece, width),
    )
    return pl.pallas_call(
        functools.partial(end_kernel, fs, float(rank * width * tp)),
        out_shape=(
            jax.ShapeDtypeStruct(weight.shape, f32),
            jax.ShapeDtypeStruct((fs * rows, width), bf16),
            jax.ShapeDtypeStruct(weight.shape, f32),
            jax.ShapeDtypeStruct(first_moment.shape, f32),
            jax.ShapeDtypeStruct(first_moment.shape, f32),
        ),
        in_specs=[vmem] * 9,
        out_specs=(vmem,) * 5,
        compiler_params=pltpu.CompilerParams(vmem_limit_bytes=32 * 1024 * 1024),
        name="end_kernel",
    )(
        sq, factor, dirs.reshape(n * piece, width), fac.reshape(fs * rows, rank),
        wbf.reshape(fs * rows, width), weight, proj.reshape(own_rows, width), first_moment, second_moment,
    )


def solution(mesh):
    sizes = (mesh.shape["fs"], mesh.shape["rep"], mesh.shape["tp"])
    in_specs = (
        P(("fs", "rep"), None),
        P(("fs", "rep"), "tp"),
        P(("fs", "rep"), "tp"),
        P(("fs", "rep"), "tp"),
        P(("fs", "rep"), "tp"),
        P("tp"),
        P("fs", None),
        P("fs", "tp"),
        P("fs", "tp"),
        P("fs", "tp"),
    )
    out_specs = (P("fs", "tp"), P(None, "tp"), P("fs", "tp"), P("fs", "tp"), P("fs", "tp"))
    return jax.shard_map(
        functools.partial(on_device, *sizes),
        mesh=mesh, in_specs=in_specs, out_specs=out_specs, check_vma=False,
    )
```

```python
import functools

import jax
import jax.numpy as jnp
from jax import lax
from jax.experimental import pallas as pl
from jax.experimental.pallas import tpu as pltpu
from jax.sharding import PartitionSpec as P

MESH = pl.DeviceIdType.MESH
LANES = 128
NT = (((1,), (1,)), ((), ()))
TN = (((0,), (0,)), ((), ()))


def attention_pair(pair, q_v, k_v, v_v, g_v, scale_ref, acc, kgb, head_width):
    length = q_v.shape[0]
    per = LANES // head_width
    block = min(LANES, length)
    cols = slice(pair * LANES, (pair + 1) * LANES)
    value_width = v_v.shape[1] // (q_v.shape[1] // head_width)
    lane = lax.broadcasted_iota(jnp.int32, (length, LANES), 1)
    tri = lax.broadcasted_iota(jnp.int32, (block, block), 0) <= lax.broadcasted_iota(
        jnp.int32, (block, block), 1
    )
    for inner_head in range(per):
        head = pair * per + inner_head
        in_head = (lane >= inner_head * head_width) & (lane < (inner_head + 1) * head_width)
        queries = jnp.where(in_head, q_v[:, cols].astype(jnp.float32) * head_width ** (-0.5), 0.0)
        queries = queries.astype(jnp.bfloat16)
        vcols = slice(head * value_width, (head + 1) * value_width)
        scale = scale_ref[head]
        for at in reversed(range(length // block)):
            keys_to = (at + 1) * block
            rows = slice(at * block, keys_to)
            qb = queries[rows]
            s = lax.dot_general(k_v[:keys_to, cols], qb, NT, preferred_element_type=jnp.float32)
            last = jnp.where(tri, s[at * block :], -1e30)
            s = last if at == 0 else jnp.concatenate([s[: at * block], last], axis=0)
            e = jnp.exp(s - jnp.max(s, axis=0, keepdims=True))
            inv = 1.0 / jnp.sum(e, axis=0, keepdims=True)
            a = lax.dot_general(
                v_v[:keys_to, vcols], g_v[rows, vcols], NT, preferred_element_type=jnp.float32
            )
            row_inner = jnp.sum(e * a, axis=0, keepdims=True) * inv
            sg = (e * (a - row_inner) * (-scale * inv)).astype(jnp.bfloat16)
            add = jnp.dot(sg, qb, preferred_element_type=jnp.float32)
            if inner_head == 0 and at == length // block - 1:
                acc[...] = add
            else:
                acc[:keys_to] += add
    kgb[:, cols] = acc[...].astype(jnp.bfloat16)


def main_kernel(
    fs, rep, tp, head_width,
    scale_h, tok_h, q_h, k_h, v_h, g_h, factor_h, weight_h, first_h, second_h,
    fac, wbf, dirs, proj, sq_out,
    scale_ref, tok, q_v, k_v, v_v, g_v, wq, wsend, fm, sm, acc, kgb, red, psend, precv, sq_own, sq_in,
    ld, fac_s, fac_r, fq_s, fq_r, fr_s, fr_r, par_s, par_r, w_s, w_r, wf_s, wf_r, pc_s, pc_r, dr_s, dr_r, pj_s, pj_r, sq_s, sq_r,
):
    n = fs * rep
    z, r, c = lax.axis_index("fs"), lax.axis_index("rep"), lax.axis_index("tp")
    me = z * rep + r
    other = lax.rem(c + 1, tp)
    partner = {"fs": z, "rep": r, "tp": other}
    half = fac.shape[2] // tp
    my_cols = pl.ds(pl.multiple_of(c * half, half), half)
    his_cols = pl.ds(pl.multiple_of(other * half, half), half)

    def remote(src, dst, send, recv, device):
        return pltpu.make_async_remote_copy(
            src_ref=src, dst_ref=dst, send_sem=send, recv_sem=recv, device_id=device, device_id_type=MESH
        )

    def fs_dev(i):
        return {"fs": i, "rep": r, "tp": c}

    def rep_dev(i):
        return {"fs": z, "rep": i, "tp": c}

    def any_dev(i):
        return {"fs": i // rep, "rep": lax.rem(i, rep), "tp": c}

    def each(count, body):
        def step(d, carry):
            body(d)
            return carry

        lax.fori_loop(1, count, step, 0)

    barrier = pltpu.get_barrier_semaphore()
    pl.semaphore_signal(barrier, inc=1, device_id=partner, device_id_type=MESH)

    def greet(d):
        pl.semaphore_signal(barrier, inc=1, device_id=any_dev(lax.rem(me + d, n)), device_id_type=MESH)

    each(n, greet)

    loads = [
        pltpu.make_async_copy(src, dst, ld.at[i])
        for i, (src, dst) in enumerate(
            [
                (factor_h, fac.at[z]), (weight_h.at[r], wq), (q_h, q_v), (k_h, k_v), (v_h, v_v), (g_h, g_v),
                (scale_h, scale_ref), (tok_h, tok), (first_h.at[r], fm), (second_h.at[r], sm),
            ]
        )
    ]
    for load in loads:
        load.start()
    loads[1].wait()
    wsend[...] = wq[...].astype(jnp.bfloat16)
    loads[0].wait()
    pl.semaphore_wait(barrier, n)

    def fac_copy(slot, sem, to):
        part = fac.at[slot, pl.ds(0, direct), my_cols]
        return remote(part, part, fac_s.at[sem], fac_r.at[slot], fs_dev(to))

    share = fac.shape[1] // (2 * rep)
    share = share if share % 16 == 0 else 0
    direct = fac.shape[1] - share * rep

    def share_rows(lane):
        return pl.ds(pl.multiple_of(direct + lane * share, 16), share)

    def fq_copy(slot, sem, to):
        part = fac.at[slot, share_rows(r), my_cols]
        return remote(part, part, fq_s.at[sem], fq_r.at[slot], fs_dev(to))

    def fr_copy(slot, lane, sem, to):
        part = fac.at[slot, share_rows(lane), my_cols]
        return remote(part, part, fr_s.at[slot, sem], fr_r.at[slot, lane], rep_dev(to))

    def relay_fac(d):
        src = lax.rem(z + d, fs)
        fq_copy(src, d, src).wait_recv()
        each(rep, lambda k: fr_copy(src, r, k, lax.rem(r + k, rep)).start())

    def wait_fac_relay(src):
        def inner(k):
            lane = lax.rem(r + k, rep)
            fr_copy(src, lane, k, lane).wait_recv()

        each(rep, inner)

    def send_fac(d):
        fac_copy(z, d, lax.rem(z + d, fs)).start()

    if share:
        each(fs, lambda d: fq_copy(z, d, lax.rem(z + d, fs)).start())
    each(fs, send_fac)

    def w_copy(slot, sem, to):
        return remote(wsend, wbf.at[slot, r], w_s.at[sem], w_r.at[slot], fs_dev(to))

    def send_w(d):
        w_copy(z, d, lax.rem(z + d, fs)).start()

    each(fs, send_w)

    for i in range(2, 7):
        loads[i].wait()
    for pair in range(q_v.shape[1] // LANES):
        attention_pair(pair, q_v, k_v, v_v, g_v, scale_ref, acc, kgb, head_width)
        if pair == 0 and share:
            each(fs, relay_fac)
    for i in range(7, 10):
        loads[i].wait()

    by_shard = fac.shape[1] % LANES == 0

    def tokens_of(j):
        return tok[:, pl.ds(pl.multiple_of(j * fac.shape[1], LANES), fac.shape[1])]

    if by_shard:
        red[...] = jnp.dot(tokens_of(z), fac[z], preferred_element_type=jnp.float32)

    def par_copy(slot, cols):
        part = fac.at[slot, :, cols]
        return remote(part, part, par_s.at[slot], par_r.at[slot], partner)

    def forward_fac(d):
        src = lax.rem(z + d, fs)
        fac_copy(src, d, src).wait_recv()
        if share:
            wait_fac_relay(src)
        par_copy(src, my_cols).start()

    each(fs, forward_fac)

    def use_fac(d):
        src = lax.rem(z + d, fs)
        par_copy(src, his_cols).wait_recv()
        if by_shard:
            red[...] += jnp.dot(tokens_of(src), fac[src], preferred_element_type=jnp.float32)

    each(fs, use_fac)
    if not by_shard:
        whole = jnp.concatenate([fac[j] for j in range(fs)], axis=0)
        red[...] = jnp.dot(tok[...], whole, preferred_element_type=jnp.float32)

    partial = lax.dot_general(
        red[...].astype(jnp.bfloat16), kgb[...], TN, preferred_element_type=jnp.float32
    )
    piece = psend.shape[1]
    for i in range(n):
        psend[i] = partial[i * piece : (i + 1) * piece].astype(jnp.bfloat16)

    def pc_copy(part, slot, sem, to):
        return remote(psend.at[part], precv.at[slot], pc_s.at[sem], pc_r.at[slot], any_dev(to))

    def send_piece(d):
        to = lax.rem(me + d, n)
        pc_copy(to, me, d, to).start()

    each(n, send_piece)

    def wf_copy(slot, lane, sem, to):
        part = wbf.at[slot, lane]
        return remote(part, part, wf_s.at[slot, sem], wf_r.at[slot, lane], rep_dev(to))

    def relay_w(d):
        src = lax.rem(z + d, fs)
        w_copy(src, d, src).wait_recv()
        each(rep, lambda k: wf_copy(src, r, k, lax.rem(r + k, rep)).start())

    each(fs, relay_w)

    def wait_piece(d):
        src = lax.rem(me + d, n)
        pc_copy(src, src, d, src).wait_recv()

    each(n, wait_piece)
    precv[me] = psend[me]
    total = jnp.sum(precv[...].astype(jnp.float32), axis=0)
    first = 0.9 * fm[...] + 0.1 * total
    second = 0.95 * sm[...] + 0.05 * total * total
    dirs[me] = (first / (jnp.sqrt(second) + 1e-08)).astype(jnp.bfloat16)
    proj[r] = total

    def dr_copy(slot, sem, to):
        part = dirs.at[slot]
        return remote(part, part, dr_s.at[sem], dr_r.at[slot], any_dev(to))

    def pj_copy(slot, sem, to):
        part = proj.at[slot]
        return remote(part, part, pj_s.at[sem], pj_r.at[slot], rep_dev(to))

    each(n, lambda d: dr_copy(me, d, lax.rem(me + d, n)).start())
    each(rep, lambda d: pj_copy(r, d, lax.rem(r + d, rep)).start())

    def wait_dir(d):
        src = lax.rem(me + d, n)
        dr_copy(src, d, src).wait_recv()

    each(n, wait_dir)
    wide = dirs[...].astype(jnp.float32)
    sq_own[...] = jnp.full(sq_own.shape, jnp.sum(wide * wide), jnp.float32)
    sq_copy = remote(sq_own, sq_in, sq_s, sq_r, partner)
    sq_copy.start()

    def wait_proj(d):
        src = lax.rem(r + d, rep)
        pj_copy(src, d, src).wait_recv()

    each(rep, wait_proj)

    def wait_relay(d):
        src = lax.rem(z + d, fs)

        def inner(k):
            lane = lax.rem(r + k, rep)
            wf_copy(src, lane, k, lane).wait_recv()

        each(rep, inner)

    each(fs, wait_relay)

    def wait_sends_fs(d):
        src = lax.rem(z + d, fs)
        fac_copy(z, d, src).wait_send()
        if share:
            fq_copy(z, d, src).wait_send()
            each(rep, lambda k: fr_copy(src, r, k, lax.rem(r + k, rep)).wait_send())
        w_copy(z, d, src).wait_send()
        par_copy(src, my_cols).wait_send()
        each(rep, lambda k: wf_copy(src, r, k, lax.rem(r + k, rep)).wait_send())

    each(fs, wait_sends_fs)

    def wait_sends_all(d):
        to = lax.rem(me + d, n)
        pc_copy(to, me, d, to).wait_send()
        dr_copy(me, d, to).wait_send()

    each(n, wait_sends_all)
    each(rep, lambda d: pj_copy(r, d, lax.rem(r + d, rep)).wait_send())
    sq_copy.wait()
    sq_out[...] = sq_own[...] + sq_in[...]


def end_kernel(
    fs, entries,
    sq, factor, direction, fac, wbf, weight, proj, fm, sm,
    new_weight, copies, update, new_first, new_second,
):
    z = lax.axis_index("fs")
    rows = factor.shape[0]
    ratio = lax.rsqrt(sq[0:1, 0:1] / entries + 1e-06)
    own = jnp.dot(factor[...], direction[...], preferred_element_type=jnp.float32) * ratio
    update[...] = own
    changed = weight[...] - 0.1 * own
    new_weight[...] = changed
    copies[pl.ds(pl.multiple_of(z * rows, rows), rows), :] = changed.astype(jnp.bfloat16)
    for d in range(1, fs):
        at = pl.ds(pl.multiple_of(lax.rem(z + d, fs) * rows, rows), rows)
        step = jnp.dot(fac[at, :], direction[...], preferred_element_type=jnp.float32) * ratio
        copies[at, :] = (wbf[at, :].astype(jnp.float32) - 0.1 * step).astype(jnp.bfloat16)
    total = proj[...]
    new_first[...] = 0.9 * fm[...] + 0.1 * total
    new_second[...] = 0.95 * sm[...] + 0.05 * total * total


def on_device(
    fs, rep, tp,
    tokens_in, query_two, key_two, values, out_grad, second_scale, factor, weight, first_moment, second_moment,
):
    n = fs * rep
    length, width = query_two.shape
    head_width = width // second_scale.shape[0]
    rows, rank = factor.shape
    own_rows = first_moment.shape[0]
    piece = own_rows // rep
    w_rows = rows // rep
    f32, bf16 = jnp.float32, jnp.bfloat16
    hbm = pl.BlockSpec(memory_space=pltpu.HBM)
    vmem = pl.BlockSpec(memory_space=pltpu.VMEM)
    dma = pltpu.SemaphoreType.DMA
    fac, wbf, dirs, proj, sq = pl.pallas_call(
        functools.partial(main_kernel, fs, rep, tp, head_width),
        out_shape=(
            jax.ShapeDtypeStruct((fs, rows, rank), bf16),
            jax.ShapeDtypeStruct((fs, rep, w_rows, width), bf16),
            jax.ShapeDtypeStruct((n, piece, width), bf16),
            jax.ShapeDtypeStruct((rep, piece, width), f32),
            jax.ShapeDtypeStruct((8, LANES), f32),
        ),
        in_specs=[hbm] * 10,
        out_specs=(vmem,) * 5,
        scratch_shapes=[
            pltpu.SMEM(second_scale.shape, f32),
            pltpu.VMEM(tokens_in.shape, bf16),
            pltpu.VMEM(query_two.shape, bf16),
            pltpu.VMEM(key_two.shape, bf16),
            pltpu.VMEM(values.shape, bf16),
            pltpu.VMEM(out_grad.shape, bf16),
            pltpu.VMEM((w_rows, width), f32),
            pltpu.VMEM((w_rows, width), bf16),
            pltpu.VMEM((piece, width), f32),
            pltpu.VMEM((piece, width), f32),
            pltpu.VMEM((length, LANES), f32),
            pltpu.VMEM((length, width), bf16),
            pltpu.VMEM((length, rank), f32),
            pltpu.VMEM((n, piece, width), bf16),
            pltpu.VMEM((n, piece, width), bf16),
            pltpu.VMEM((8, LANES), f32),
            pltpu.VMEM((8, LANES), f32),
            dma((10,)),
            dma((fs,)), dma((fs,)),
            dma((fs,)), dma((fs,)), dma((fs, rep)), dma((fs, rep)),
            dma((fs,)), dma((fs,)),
            dma((fs,)), dma((fs,)),
            dma((fs, rep)), dma((fs, rep)),
            dma((n,)), dma((n,)),
            dma((n,)), dma((n,)),
            dma((rep,)), dma((rep,)),
            dma, dma,
        ],
        compiler_params=pltpu.CompilerParams(
            collective_id=0, has_side_effects=True, vmem_limit_bytes=60 * 1024 * 1024
        ),
        name="main_kernel",
    )(
        second_scale, tokens_in, query_two, key_two, values, out_grad, factor,
        weight.reshape(rep, w_rows, width),
        first_moment.reshape(rep, piece, width),
        second_moment.reshape(rep, piece, width),
    )
    return pl.pallas_call(
        functools.partial(end_kernel, fs, float(rank * width * tp)),
        out_shape=(
            jax.ShapeDtypeStruct(weight.shape, f32),
            jax.ShapeDtypeStruct((fs * rows, width), bf16),
            jax.ShapeDtypeStruct(weight.shape, f32),
            jax.ShapeDtypeStruct(first_moment.shape, f32),
            jax.ShapeDtypeStruct(first_moment.shape, f32),
        ),
        in_specs=[vmem] * 9,
        out_specs=(vmem,) * 5,
        compiler_params=pltpu.CompilerParams(vmem_limit_bytes=60 * 1024 * 1024),
        name="end_kernel",
    )(
        sq, factor, dirs.reshape(n * piece, width), fac.reshape(fs * rows, rank),
        wbf.reshape(fs * rows, width), weight, proj.reshape(own_rows, width), first_moment, second_moment,
    )


def solution(mesh):
    sizes = (mesh.shape["fs"], mesh.shape["rep"], mesh.shape["tp"])
    in_specs = (
        P(("fs", "rep"), None),
        P(("fs", "rep"), "tp"),
        P(("fs", "rep"), "tp"),
        P(("fs", "rep"), "tp"),
        P(("fs", "rep"), "tp"),
        P("tp"),
        P("fs", None),
        P("fs", "tp"),
        P("fs", "tp"),
        P("fs", "tp"),
    )
    out_specs = (P("fs", "tp"), P(None, "tp"), P("fs", "tp"), P("fs", "tp"), P("fs", "tp"))
    return jax.shard_map(
        functools.partial(on_device, *sizes),
        mesh=mesh, in_specs=in_specs, out_specs=out_specs, check_vma=False,
    )
```

```python
import functools

import jax
import jax.numpy as jnp
from jax import lax
from jax.experimental import pallas as pl
from jax.experimental.pallas import tpu as pltpu
from jax.sharding import PartitionSpec as P

MESH = pl.DeviceIdType.MESH
LANES = 128
NT = (((1,), (1,)), ((), ()))
TN = (((0,), (0,)), ((), ()))


def attention_pair(pair, q_v, k_v, v_v, g_v, scale_ref, acc, kgb, head_width):
    length = q_v.shape[0]
    per = LANES // head_width
    block = min(LANES, length)
    cols = slice(pair * LANES, (pair + 1) * LANES)
    value_width = v_v.shape[1] // (q_v.shape[1] // head_width)
    lane = lax.broadcasted_iota(jnp.int32, (length, LANES), 1)
    tri = lax.broadcasted_iota(jnp.int32, (block, block), 0) <= lax.broadcasted_iota(
        jnp.int32, (block, block), 1
    )
    for inner_head in range(per):
        head = pair * per + inner_head
        in_head = (lane >= inner_head * head_width) & (lane < (inner_head + 1) * head_width)
        queries = jnp.where(in_head, q_v[:, cols].astype(jnp.float32) * head_width ** (-0.5), 0.0)
        queries = queries.astype(jnp.bfloat16)
        vcols = slice(head * value_width, (head + 1) * value_width)
        scale = scale_ref[head]
        for at in reversed(range(length // block)):
            keys_to = (at + 1) * block
            rows = slice(at * block, keys_to)
            qb = queries[rows]
            s = lax.dot_general(k_v[:keys_to, cols], qb, NT, preferred_element_type=jnp.float32)
            last = jnp.where(tri, s[at * block :], -1e30)
            s = last if at == 0 else jnp.concatenate([s[: at * block], last], axis=0)
            e = jnp.exp(s - jnp.max(s, axis=0, keepdims=True))
            inv = 1.0 / jnp.sum(e, axis=0, keepdims=True)
            a = lax.dot_general(
                v_v[:keys_to, vcols], g_v[rows, vcols], NT, preferred_element_type=jnp.float32
            )
            row_inner = jnp.sum(e * a, axis=0, keepdims=True) * inv
            sg = (e * (a - row_inner) * (-scale * inv)).astype(jnp.bfloat16)
            add = jnp.dot(sg, qb, preferred_element_type=jnp.float32)
            if inner_head == 0 and at == length // block - 1:
                acc[...] = add
            else:
                acc[:keys_to] += add
    kgb[:, cols] = acc[...].astype(jnp.bfloat16)


def main_kernel(
    fs, rep, tp, head_width,
    scale_h, tok_h, q_h, k_h, v_h, g_h, factor_h, weight_h, first_h, second_h,
    fac_o, wbf_o, dirs, proj, sq_out,
    fac, wbf, scale_ref, tok, q_v, k_v, v_v, g_v, wq, wsend, fm, sm, acc, kgb, red, psend, precv, sq_own, sq_in,
    ld, fac_s, fac_r, fq_s, fq_r, fr_s, fr_r, par_s, par_r, w_s, w_r, wf_s, wf_r, pc_s, pc_r, dr_s, dr_r, pj_s, pj_r, sq_s, sq_r,
):
    n = fs * rep
    z, r, c = lax.axis_index("fs"), lax.axis_index("rep"), lax.axis_index("tp")
    me = z * rep + r
    other = lax.rem(c + 1, tp)
    partner = {"fs": z, "rep": r, "tp": other}
    half = fac.shape[2] // tp
    my_cols = pl.ds(pl.multiple_of(c * half, half), half)
    his_cols = pl.ds(pl.multiple_of(other * half, half), half)

    def remote(src, dst, send, recv, device):
        return pltpu.make_async_remote_copy(
            src_ref=src, dst_ref=dst, send_sem=send, recv_sem=recv, device_id=device, device_id_type=MESH
        )

    def fs_dev(i):
        return {"fs": i, "rep": r, "tp": c}

    def rep_dev(i):
        return {"fs": z, "rep": i, "tp": c}

    def any_dev(i):
        return {"fs": i // rep, "rep": lax.rem(i, rep), "tp": c}

    def each(count, body):
        def step(d, carry):
            body(d)
            return carry

        lax.fori_loop(1, count, step, 0)

    barrier = pltpu.get_barrier_semaphore()
    pl.semaphore_signal(barrier, inc=1, device_id=partner, device_id_type=MESH)

    def greet(d):
        pl.semaphore_signal(barrier, inc=1, device_id=any_dev(lax.rem(me + d, n)), device_id_type=MESH)

    each(n, greet)

    loads = [
        pltpu.make_async_copy(src, dst, ld.at[i])
        for i, (src, dst) in enumerate(
            [
                (factor_h, fac.at[z]), (weight_h.at[r], wq), (q_h, q_v), (k_h, k_v), (v_h, v_v), (g_h, g_v),
                (scale_h, scale_ref), (tok_h, tok), (first_h.at[r], fm), (second_h.at[r], sm),
            ]
        )
    ]
    for load in loads:
        load.start()
    loads[1].wait()
    wsend[...] = wq[...].astype(jnp.bfloat16)
    loads[0].wait()
    pl.semaphore_wait(barrier, n)

    def fac_copy(slot, sem, to):
        part = fac.at[slot, pl.ds(0, direct), my_cols]
        return remote(part, part, fac_s.at[sem], fac_r.at[slot], fs_dev(to))

    share = (fac.shape[1] * 3) // (4 * rep)
    share = share if share % 16 == 0 else 0
    direct = fac.shape[1] - share * rep

    def share_rows(lane):
        return pl.ds(pl.multiple_of(direct + lane * share, 16), share)

    def fq_copy(slot, sem, to):
        part = fac.at[slot, share_rows(r), my_cols]
        return remote(part, part, fq_s.at[sem], fq_r.at[slot], fs_dev(to))

    def fr_copy(slot, lane, sem, to):
        part = fac.at[slot, share_rows(lane), my_cols]
        return remote(part, part, fr_s.at[slot, sem], fr_r.at[slot, lane], rep_dev(to))

    def relay_fac(d):
        src = lax.rem(z + d, fs)
        fq_copy(src, d, src).wait_recv()
        each(rep, lambda k: fr_copy(src, r, k, lax.rem(r + k, rep)).start())

    def wait_fac_relay(src):
        def inner(k):
            lane = lax.rem(r + k, rep)
            fr_copy(src, lane, k, lane).wait_recv()

        each(rep, inner)

    def send_fac(d):
        fac_copy(z, d, lax.rem(z + d, fs)).start()

    if share:
        each(fs, lambda d: fq_copy(z, d, lax.rem(z + d, fs)).start())
    each(fs, send_fac)

    def w_copy(slot, sem, to):
        return remote(wsend, wbf.at[slot, r], w_s.at[sem], w_r.at[slot], fs_dev(to))

    def send_w(d):
        w_copy(z, d, lax.rem(z + d, fs)).start()

    each(fs, send_w)

    for i in range(2, 7):
        loads[i].wait()
    for pair in range(q_v.shape[1] // LANES):
        attention_pair(pair, q_v, k_v, v_v, g_v, scale_ref, acc, kgb, head_width)
        if pair == 0 and share:
            each(fs, relay_fac)
    for i in range(7, 10):
        loads[i].wait()

    by_shard = fac.shape[1] % LANES == 0

    def tokens_of(j):
        return tok[:, pl.ds(pl.multiple_of(j * fac.shape[1], LANES), fac.shape[1])]

    if by_shard:
        red[...] = jnp.dot(tokens_of(z), fac[z], preferred_element_type=jnp.float32)

    def par_copy(slot, cols):
        part = fac.at[slot, :, cols]
        return remote(part, part, par_s.at[slot], par_r.at[slot], partner)

    def forward_fac(d):
        src = lax.rem(z + d, fs)
        fac_copy(src, d, src).wait_recv()
        if share:
            wait_fac_relay(src)
        par_copy(src, my_cols).start()

    each(fs, forward_fac)

    def use_fac(d):
        src = lax.rem(z + d, fs)
        par_copy(src, his_cols).wait_recv()
        if by_shard:
            red[...] += jnp.dot(tokens_of(src), fac[src], preferred_element_type=jnp.float32)

    each(fs, use_fac)
    if not by_shard:
        whole = jnp.concatenate([fac[j] for j in range(fs)], axis=0)
        red[...] = jnp.dot(tok[...], whole, preferred_element_type=jnp.float32)

    fac_out = pltpu.make_async_copy(fac, fac_o, ld.at[10])
    fac_out.start()
    partial = lax.dot_general(
        red[...].astype(jnp.bfloat16), kgb[...], TN, preferred_element_type=jnp.float32
    )
    piece = psend.shape[1]
    for i in range(n):
        psend[i] = partial[i * piece : (i + 1) * piece].astype(jnp.bfloat16)

    def pc_copy(part, slot, sem, to):
        return remote(psend.at[part], precv.at[slot], pc_s.at[sem], pc_r.at[slot], any_dev(to))

    def send_piece(d):
        to = lax.rem(me + d, n)
        pc_copy(to, me, d, to).start()

    each(n, send_piece)

    def wf_copy(slot, lane, sem, to):
        part = wbf.at[slot, lane]
        return remote(part, part, wf_s.at[slot, sem], wf_r.at[slot, lane], rep_dev(to))

    def relay_w(d):
        src = lax.rem(z + d, fs)
        w_copy(src, d, src).wait_recv()
        each(rep, lambda k: wf_copy(src, r, k, lax.rem(r + k, rep)).start())

    each(fs, relay_w)

    def wait_piece(d):
        src = lax.rem(me + d, n)
        pc_copy(src, src, d, src).wait_recv()

    each(n, wait_piece)
    precv[me] = psend[me]
    total = jnp.sum(precv[...].astype(jnp.float32), axis=0)
    first = 0.9 * fm[...] + 0.1 * total
    second = 0.95 * sm[...] + 0.05 * total * total
    dirs[me] = (first / (jnp.sqrt(second) + 1e-08)).astype(jnp.bfloat16)
    proj[r] = total

    def dr_copy(slot, sem, to):
        part = dirs.at[slot]
        return remote(part, part, dr_s.at[sem], dr_r.at[slot], any_dev(to))

    def pj_copy(slot, sem, to):
        part = proj.at[slot]
        return remote(part, part, pj_s.at[sem], pj_r.at[slot], rep_dev(to))

    each(n, lambda d: dr_copy(me, d, lax.rem(me + d, n)).start())
    each(rep, lambda d: pj_copy(r, d, lax.rem(r + d, rep)).start())

    def wait_dir(d):
        src = lax.rem(me + d, n)
        dr_copy(src, d, src).wait_recv()

    each(n, wait_dir)
    wide = dirs[...].astype(jnp.float32)
    sq_own[...] = jnp.full(sq_own.shape, jnp.sum(wide * wide), jnp.float32)
    sq_copy = remote(sq_own, sq_in, sq_s, sq_r, partner)
    sq_copy.start()

    def wait_proj(d):
        src = lax.rem(r + d, rep)
        pj_copy(src, d, src).wait_recv()

    each(rep, wait_proj)

    def wait_relay(d):
        src = lax.rem(z + d, fs)

        def inner(k):
            lane = lax.rem(r + k, rep)
            wf_copy(src, lane, k, lane).wait_recv()

        each(rep, inner)

    each(fs, wait_relay)

    wbf[z] = jnp.zeros(wbf.shape[1:], jnp.bfloat16)
    wbf_out = pltpu.make_async_copy(wbf, wbf_o, ld.at[11])
    wbf_out.start()

    def wait_sends_fs(d):
        src = lax.rem(z + d, fs)
        fac_copy(z, d, src).wait_send()
        if share:
            fq_copy(z, d, src).wait_send()
            each(rep, lambda k: fr_copy(src, r, k, lax.rem(r + k, rep)).wait_send())
        w_copy(z, d, src).wait_send()
        par_copy(src, my_cols).wait_send()
        each(rep, lambda k: wf_copy(src, r, k, lax.rem(r + k, rep)).wait_send())

    each(fs, wait_sends_fs)

    def wait_sends_all(d):
        to = lax.rem(me + d, n)
        pc_copy(to, me, d, to).wait_send()
        dr_copy(me, d, to).wait_send()

    each(n, wait_sends_all)
    each(rep, lambda d: pj_copy(r, d, lax.rem(r + d, rep)).wait_send())
    sq_copy.wait()
    fac_out.wait()
    wbf_out.wait()
    sq_out[...] = sq_own[...] + sq_in[...]


def end_kernel(
    fs, entries,
    sq, factor, direction, fac, wbf, weight, proj, fm, sm,
    new_weight, copies, update, new_first, new_second,
):
    z = lax.axis_index("fs")
    rows = factor.shape[0]
    ratio = lax.rsqrt(sq[0:1, 0:1] / entries + 1e-06)
    own = jnp.dot(factor[...], direction[...], preferred_element_type=jnp.float32) * ratio
    update[...] = own
    changed = weight[...] - 0.1 * own
    new_weight[...] = changed
    copies[pl.ds(pl.multiple_of(z * rows, rows), rows), :] = changed.astype(jnp.bfloat16)
    for d in range(1, fs):
        at = pl.ds(pl.multiple_of(lax.rem(z + d, fs) * rows, rows), rows)
        step = jnp.dot(fac[at, :], direction[...], preferred_element_type=jnp.float32) * ratio
        copies[at, :] = (wbf[at, :].astype(jnp.float32) - 0.1 * step).astype(jnp.bfloat16)
    total = proj[...]
    new_first[...] = 0.9 * fm[...] + 0.1 * total
    new_second[...] = 0.95 * sm[...] + 0.05 * total * total


def on_device(
    fs, rep, tp,
    tokens_in, query_two, key_two, values, out_grad, second_scale, factor, weight, first_moment, second_moment,
):
    n = fs * rep
    length, width = query_two.shape
    head_width = width // second_scale.shape[0]
    rows, rank = factor.shape
    own_rows = first_moment.shape[0]
    piece = own_rows // rep
    w_rows = rows // rep
    f32, bf16 = jnp.float32, jnp.bfloat16
    hbm = pl.BlockSpec(memory_space=pltpu.HBM)
    vmem = pl.BlockSpec(memory_space=pltpu.VMEM)
    dma = pltpu.SemaphoreType.DMA
    fac, wbf, dirs, proj, sq = pl.pallas_call(
        functools.partial(main_kernel, fs, rep, tp, head_width),
        out_shape=(
            jax.ShapeDtypeStruct((fs, rows, rank), bf16),
            jax.ShapeDtypeStruct((fs, rep, w_rows, width), bf16),
            jax.ShapeDtypeStruct((n, piece, width), bf16),
            jax.ShapeDtypeStruct((rep, piece, width), f32),
            jax.ShapeDtypeStruct((8, LANES), f32),
        ),
        in_specs=[hbm] * 10,
        out_specs=(hbm, hbm, vmem, vmem, vmem),
        scratch_shapes=[
            pltpu.VMEM((fs, rows, rank), bf16),
            pltpu.VMEM((fs, rep, w_rows, width), bf16),
            pltpu.SMEM(second_scale.shape, f32),
            pltpu.VMEM(tokens_in.shape, bf16),
            pltpu.VMEM(query_two.shape, bf16),
            pltpu.VMEM(key_two.shape, bf16),
            pltpu.VMEM(values.shape, bf16),
            pltpu.VMEM(out_grad.shape, bf16),
            pltpu.VMEM((w_rows, width), f32),
            pltpu.VMEM((w_rows, width), bf16),
            pltpu.VMEM((piece, width), f32),
            pltpu.VMEM((piece, width), f32),
            pltpu.VMEM((length, LANES), f32),
            pltpu.VMEM((length, width), bf16),
            pltpu.VMEM((length, rank), f32),
            pltpu.VMEM((n, piece, width), bf16),
            pltpu.VMEM((n, piece, width), bf16),
            pltpu.VMEM((8, LANES), f32),
            pltpu.VMEM((8, LANES), f32),
            dma((12,)),
            dma((fs,)), dma((fs,)),
            dma((fs,)), dma((fs,)), dma((fs, rep)), dma((fs, rep)),
            dma((fs,)), dma((fs,)),
            dma((fs,)), dma((fs,)),
            dma((fs, rep)), dma((fs, rep)),
            dma((n,)), dma((n,)),
            dma((n,)), dma((n,)),
            dma((rep,)), dma((rep,)),
            dma, dma,
        ],
        compiler_params=pltpu.CompilerParams(
            collective_id=0, has_side_effects=True, vmem_limit_bytes=60 * 1024 * 1024
        ),
        name="main_kernel",
    )(
        second_scale, tokens_in, query_two, key_two, values, out_grad, factor,
        weight.reshape(rep, w_rows, width),
        first_moment.reshape(rep, piece, width),
        second_moment.reshape(rep, piece, width),
    )
    return pl.pallas_call(
        functools.partial(end_kernel, fs, float(rank * width * tp)),
        out_shape=(
            jax.ShapeDtypeStruct(weight.shape, f32),
            jax.ShapeDtypeStruct((fs * rows, width), bf16),
            jax.ShapeDtypeStruct(weight.shape, f32),
            jax.ShapeDtypeStruct(first_moment.shape, f32),
            jax.ShapeDtypeStruct(first_moment.shape, f32),
        ),
        in_specs=[vmem] * 9,
        out_specs=(vmem,) * 5,
        compiler_params=pltpu.CompilerParams(vmem_limit_bytes=60 * 1024 * 1024),
        name="end_kernel",
    )(
        sq, factor, dirs.reshape(n * piece, width), fac.reshape(fs * rows, rank),
        wbf.reshape(fs * rows, width), weight, proj.reshape(own_rows, width), first_moment, second_moment,
    )


def solution(mesh):
    sizes = (mesh.shape["fs"], mesh.shape["rep"], mesh.shape["tp"])
    in_specs = (
        P(("fs", "rep"), None),
        P(("fs", "rep"), "tp"),
        P(("fs", "rep"), "tp"),
        P(("fs", "rep"), "tp"),
        P(("fs", "rep"), "tp"),
        P("tp"),
        P("fs", None),
        P("fs", "tp"),
        P("fs", "tp"),
        P("fs", "tp"),
    )
    out_specs = (P("fs", "tp"), P(None, "tp"), P("fs", "tp"), P("fs", "tp"), P("fs", "tp"))
    return jax.shard_map(
        functools.partial(on_device, *sizes),
        mesh=mesh, in_specs=in_specs, out_specs=out_specs, check_vma=False,
    )
```
